32 devices in a mesh: sp: 8 (over z, y), tp: 4 (over x, core).
Axes of the slice: x: 2, y: 2, z: 4, core: 2. Of those that a mesh axis runs over, the one named last changes fastest.
Arguments:
- queries: bfloat16 [1024, 1280], P('sp', 'tp'), may hold values from -4000 to 4000
- latents: bfloat16 [1024, 512], P('sp'), may hold values from -6 to 6
- shared_key: bfloat16 [1024, 64], P('sp'), may hold values from -4 to 4
- expand_weight: bfloat16 [512, 1536], P(None, 'tp'), may hold values from -0.25 to 0.25
- residual: bfloat16 [1024, 2048], P('sp'), may hold values from -3 to 3
- out_weight: bfloat16 [768, 2048], replicated, may hold values from -0.21875 to 0.21875
- norm_gain: bfloat16 [2048], replicated, may hold values from 0.099609375 to 1.8984375
- gate_weight: bfloat16 [2048, 3072], P('sp', 'tp'), may hold values from -0.125 to 0.125
- value_weight: bfloat16 [2048, 3072], P('sp', 'tp'), may hold values from -0.125 to 0.125
- conv_weight: bfloat16 [3, 3072], P(None, 'tp'), may hold values from -3.5 to 3.5
- down_weight: bfloat16 [3072, 2048], P('tp', 'sp'), may hold values from -0.109375 to 0.109375
Outputs:
- output: bfloat16 [1024, 2048], P(('sp', 'tp'))
The draws below stay inside these ranges and needn't reach their ends.
All inputs are finite; a program needn't handle non-finite values.
Results may differ from the reference program's by a relative error of at most 0.018.
Values may be sent and summed in bfloat16 or wider, within the bound.
A program may use at most 128 MiB of HBM per device.

```python
import jax
import jax.numpy as jnp
from jax import lax

D = 2048
HEADS = 4
NOPE_A = 128
VAL_A = 128
NOPE_B = 64
VAL_B = 64
ROPE = 64
RANK = 512
FF = 3072
CONV = 3
TOK_DEV = 128
TOKENS = 1024


def shared_rows(key):
    drawn = jax.random.normal(jax.random.fold_in(key, 11), (TOKENS, ROPE), jnp.float32)
    return jnp.clip(drawn, -4.0, 4.0).astype(jnp.float32)


def draw_shared_key(key, part):
    return shared_rows(key).reshape(TOKENS, ROPE).astype(jnp.bfloat16)


def draw_queries(key, part):
    q_width = NOPE_A + NOPE_B + 2 * ROPE
    base_draw = jnp.clip(3.0 * jax.random.normal(jax.random.fold_in(key, 23), (TOKENS, HEADS, q_width), jnp.float32), -18.0, 18.0)
    return jnp.clip(base_draw, -4000.0, 4000.0).reshape(TOKENS, HEADS * q_width).astype(jnp.bfloat16)


def steps_of(own_key, extent, pieces, low, high):
    gain, own = 1.0, jax.random.fold_in(own_key, 6)
    for dim, parts in pieces:
        heights = jnp.exp(jax.random.uniform(jax.random.fold_in(own, dim), (parts,), jnp.float32, low / len(pieces), high / len(pieces)))
        gain = gain * jnp.repeat(heights, extent[dim] // parts).reshape([-1 if axis == dim else 1 for axis in range(len(extent))])
    return gain


def noise(stream_key, shape, deviation, limit, pieces=(), held_as=jnp.bfloat16):
    array = jax.random.normal(stream_key, shape, jnp.float32) * deviation
    if len(pieces) > 0:
        array = steps_of(stream_key, shape, pieces, -0.22, 0.18) * array
    return jnp.clip(array, min=-limit, max=limit).astype(held_as)


def setup_inputs(seed: int = 0) -> dict:
    key_of = jax.random.split(jax.random.key(seed), 12)
    return {
        "queries": draw_queries(jax.random.fold_in(key_of[11], 71), 0),
        "latents": noise(key_of[1], (TOKENS, RANK), 1.0, 6.0, ((0, 8),)),
        "shared_key": draw_shared_key(jax.random.fold_in(key_of[11], 71), 0),
        "expand_weight": noise(key_of[3], (RANK, HEADS * (NOPE_A + VAL_A + NOPE_B + VAL_B)), RANK ** -0.5, 0.25, ((1, 4),)),
        "residual": noise(key_of[4], (TOKENS, D), 0.5, 3.0, ((0, 8),)),
        "out_weight": noise(key_of[5], (HEADS * (VAL_A + VAL_B), D), (HEADS * (VAL_A + VAL_B)) ** -0.5, 0.21875),
        "norm_gain": jnp.clip(1.0 + 0.18 * jax.random.normal(key_of[6], (D,), jnp.float32), 0.099609375, 1.8984375).astype(jnp.bfloat16),
        "gate_weight": noise(key_of[7], (D, FF), D ** -0.5, 0.125, ((0, 8), (1, 4))),
        "value_weight": noise(key_of[8], (D, FF), D ** -0.5, 0.125, ((0, 8), (1, 4))),
        "conv_weight": noise(key_of[9], (CONV, FF), CONV ** -0.5, 3.5, ((1, 4),)),
        "down_weight": noise(key_of[10], (FF, D), FF ** -0.5, 0.109375, ((0, 4), (1, 8))),
    }


def tables(positions, width):
    half_width = width // 2
    frequency = 10000.0 ** (-jnp.arange(half_width, dtype=jnp.float32) / half_width)
    angles = positions.astype(jnp.float32)[:, None] * frequency[None, :]
    return (jnp.cos(angles), jnp.sin(angles))

def rotate(vectors, cos_table, sine_table):
    half_width = vectors.shape[-1] // 2
    first_half = vectors[:, :half_width].astype(jnp.float32)
    second_half = vectors[:, half_width:].astype(jnp.float32)
    turned = jnp.concatenate([first_half * cos_table - second_half * sine_table, second_half * cos_table + first_half * sine_table], axis=1)
    return turned.astype(jnp.bfloat16)

def attend_head(q_content, q_turned, k_content, k_turned, values, score_scale):
    tokens = q_content.shape[0]
    blocks = tokens // TOK_DEV

    def one_block(block_index):
        first_row = (block_index * TOK_DEV).astype(jnp.int32)
        content = lax.dynamic_slice_in_dim(q_content, first_row, TOK_DEV, 0)
        rotary = lax.dynamic_slice_in_dim(q_turned, first_row, TOK_DEV, 0)
        scores = (jnp.dot(content, k_content.T, preferred_element_type=jnp.float32) + jnp.dot(rotary, k_turned.T, preferred_element_type=jnp.float32)) * score_scale
        row_max = lax.optimization_barrier(jnp.max(scores, axis=1, keepdims=True))
        weights = jnp.exp(scores - row_max)
        row_sum = lax.optimization_barrier(jnp.sum(weights, axis=1, keepdims=True))
        weighted = jnp.dot(weights.astype(jnp.bfloat16), values, preferred_element_type=jnp.float32)
        return (weighted / row_sum).astype(jnp.bfloat16)
    result = lax.map(one_block, jnp.arange(blocks, dtype=jnp.int32))
    return result.reshape(tokens, values.shape[1])

def reference(queries, latents, shared_key, expand_weight, residual, out_weight, norm_gain, gate_weight, value_weight, conv_weight, down_weight):
    tokens = queries.shape[0]
    q_width = NOPE_A + NOPE_B + 2 * ROPE
    kv_width = NOPE_A + VAL_A + NOPE_B + VAL_B
    cos_table, sine_table = tables(jnp.arange(tokens, dtype=jnp.int32), ROPE)
    key_turned = rotate(shared_key, cos_table, sine_table)
    expanded = jnp.dot(latents, expand_weight, preferred_element_type=jnp.float32).astype(jnp.bfloat16)
    scale_wide = (NOPE_A + ROPE) ** (-0.5)
    scale_narrow = (NOPE_B + ROPE) ** (-0.5)
    outputs = []
    for pair_index in range(HEADS):
        q_base = pair_index * q_width
        kv_base = pair_index * kv_width
        wide_content = queries[:, q_base:q_base + NOPE_A]
        narrow_content = queries[:, q_base + NOPE_A:q_base + NOPE_A + NOPE_B]
        rotary_base = q_base + NOPE_A + NOPE_B
        wide_turned = rotate(queries[:, rotary_base:rotary_base + ROPE], cos_table, sine_table)
        narrow_turned = rotate(queries[:, rotary_base + ROPE:rotary_base + 2 * ROPE], cos_table, sine_table)
        wide_keys = expanded[:, kv_base:kv_base + NOPE_A]
        wide_values = expanded[:, kv_base + NOPE_A:kv_base + NOPE_A + VAL_A]
        narrow_base = kv_base + NOPE_A + VAL_A
        narrow_keys = expanded[:, narrow_base:narrow_base + NOPE_B]
        narrow_values = expanded[:, narrow_base + NOPE_B:narrow_base + NOPE_B + VAL_B]
        outputs.append(attend_head(wide_content, wide_turned, wide_keys, key_turned, wide_values, scale_wide))
        outputs.append(attend_head(narrow_content, narrow_turned, narrow_keys, key_turned, narrow_values, scale_narrow))
    attended = jnp.concatenate(outputs, axis=1)
    projected = jnp.dot(attended, out_weight, preferred_element_type=jnp.float32)
    stream = (residual.astype(jnp.float32) + projected).astype(jnp.bfloat16)
    stream_f = stream.astype(jnp.float32)
    scaled = stream_f * lax.rsqrt(lax.optimization_barrier(jnp.mean(stream_f * stream_f, axis=1, keepdims=True)) + 1e-06)
    normed = (scaled * norm_gain.astype(jnp.float32)).astype(jnp.bfloat16)
    gate_pre = jnp.dot(normed, gate_weight, preferred_element_type=jnp.float32).astype(jnp.bfloat16)
    value_pre = jnp.dot(normed, value_weight, preferred_element_type=jnp.float32).astype(jnp.bfloat16)
    reach = CONV // 2
    padded = jnp.pad(gate_pre, ((reach, reach), (0, 0)))
    mixed_gate = jnp.zeros(gate_pre.shape, jnp.float32)
    for tap in range(CONV):
        mixed_gate = mixed_gate + padded[tap:tap + tokens].astype(jnp.float32) * conv_weight[tap].astype(jnp.float32)
    active = (jax.nn.silu(mixed_gate) * value_pre.astype(jnp.float32)).astype(jnp.bfloat16)
    down = jnp.dot(active, down_weight, preferred_element_type=jnp.float32)
    return (stream.astype(jnp.float32) + down).astype(jnp.bfloat16)
```

```python
import functools

import jax
import jax.numpy as jnp
from jax import lax
from jax.experimental import pallas as pl
from jax.experimental.pallas import tpu as pltpu
from jax.sharding import PartitionSpec as P

NOPE_A = 128
VAL_A = 128
NOPE_B = 64
VAL_B = 64
ROPE = 64


def padded_2(block, sides, width):
    for axis, dim in sides:
        count = lax.axis_size(axis)
        forward = [(i, i + 1) for i in range(count - 1)]
        backward = [(target, source) for source, target in forward]
        low = lax.ppermute(
            lax.slice_in_dim(block, block.shape[dim] - width, None, axis=dim), axis, forward
        )
        high = lax.ppermute(lax.slice_in_dim(block, 0, width, axis=dim), axis, backward)
        block = jnp.concatenate([low, block, high], axis=dim)
    return block


def tables(positions, width):
    half_width = width // 2
    frequency = 10000.0 ** (-jnp.arange(half_width, dtype=jnp.float32) / half_width)
    angles = positions.astype(jnp.float32)[:, None] * frequency[None, :]
    return (jnp.cos(angles), jnp.sin(angles))


def rotate(vectors, cos_table, sine_table):
    half_width = vectors.shape[-1] // 2
    first_half = vectors[:, :half_width].astype(jnp.float32)
    second_half = vectors[:, half_width:].astype(jnp.float32)
    turned = jnp.concatenate(
        [
            first_half * cos_table - second_half * sine_table,
            second_half * cos_table + first_half * sine_table,
        ],
        axis=1,
    )
    return turned.astype(jnp.bfloat16)


def normalize(stream, norm_gain):
    stream_f = stream.astype(jnp.float32)
    scaled = stream_f * lax.rsqrt(jnp.mean(stream_f * stream_f, axis=1, keepdims=True) + 1e-06)
    return (scaled * norm_gain.astype(jnp.float32)).astype(jnp.bfloat16)


def update(running, q_content, q_turned, k_content, k_turned, values, score_scale):
    row_max, row_sum, weighted = running
    scores = (
        jnp.einsum("qd,kd->qk", q_content, k_content, preferred_element_type=jnp.float32)
        + jnp.einsum("qd,kd->qk", q_turned, k_turned, preferred_element_type=jnp.float32)
    ) * score_scale
    new_max = jnp.maximum(row_max, jnp.max(scores, axis=1))
    weights = jnp.exp(scores - new_max[:, None])
    row_sum = jnp.sum(weights, axis=1)
    weighted = jnp.dot(weights.astype(jnp.bfloat16), values, preferred_element_type=jnp.float32)
    return (new_max, row_sum, weighted)


def body(
    queries,
    latents,
    shared_key,
    expand_weight,
    residual,
    out_weight,
    norm_gain,
    gate_weight,
    value_weight,
    conv_weight,
    down_weight,
):
    tok_rows = queries.shape[0]
    q_width = NOPE_A + NOPE_B + 2 * ROPE
    kv_width = NOPE_A + VAL_A + NOPE_B + VAL_B
    positions = lax.axis_index("sp") * tok_rows + jnp.arange(tok_rows, dtype=jnp.int32)
    cos_table, sine_table = tables(positions, ROPE)
    key_turned = rotate(shared_key, cos_table, sine_table)
    scale_wide = (NOPE_A + ROPE) ** (-0.5)
    scale_narrow = (NOPE_B + ROPE) ** (-0.5)
    initial = []
    pair_index = 0
    q_base = pair_index * q_width
    rotary_base = q_base + NOPE_A + NOPE_B
    wide_content = queries[:, q_base : q_base + NOPE_A]
    narrow_content = queries[:, q_base + NOPE_A : rotary_base]
    wide_turned = rotate(queries[:, rotary_base : rotary_base + ROPE], cos_table, sine_table)
    narrow_turned = rotate(
        queries[:, rotary_base + ROPE : rotary_base + 2 * ROPE], cos_table, sine_table
    )
    query_parts = [(wide_content, wide_turned, narrow_content, narrow_turned)]
    lowest = jnp.full((tok_rows,), -1e30, jnp.float32)
    empty_sum = jnp.zeros((tok_rows,), jnp.float32)
    initial += [
        lowest,
        empty_sum,
        jnp.zeros((tok_rows, VAL_A), jnp.float32),
        lowest,
        empty_sum,
        jnp.zeros((tok_rows, VAL_B), jnp.float32),
    ]
    initial = tuple(initial)
    pieces = (
        lax.all_gather(latents, "sp", axis=0, tiled=True),
        lax.all_gather(key_turned, "sp", axis=0, tiled=True),
    )
    expanded = jnp.dot(pieces[0], expand_weight, preferred_element_type=jnp.float32).astype(
        jnp.bfloat16
    )
    turned_keys = pieces[1]
    result = []
    pair_index = 0
    wide_content, wide_turned, narrow_content, narrow_turned = query_parts[pair_index]
    kv_base = pair_index * kv_width
    narrow_base = kv_base + NOPE_A + VAL_A
    wide_keys = expanded[:, kv_base : kv_base + NOPE_A]
    wide_values = expanded[:, kv_base + NOPE_A : narrow_base]
    narrow_keys = expanded[:, narrow_base : narrow_base + NOPE_B]
    narrow_values = expanded[:, narrow_base + NOPE_B : narrow_base + NOPE_B + VAL_B]
    absorb_offset = 6 * pair_index
    result += list(
        update(
            initial[absorb_offset : absorb_offset + 3],
            wide_content,
            wide_turned,
            wide_keys,
            turned_keys,
            wide_values,
            scale_wide,
        )
    )
    result += list(
        update(
            initial[absorb_offset + 3 : absorb_offset + 6],
            narrow_content,
            narrow_turned,
            narrow_keys,
            turned_keys,
            narrow_values,
            scale_narrow,
        )
    )
    running = tuple(result)
    outputs = []
    pair_index = 0
    for group_index in range(2):
        offset = 6 * pair_index + 3 * group_index
        outputs.append((running[offset + 2] / running[offset + 1][:, None]).astype(jnp.bfloat16))
    attended = jnp.concatenate(outputs, axis=1)
    share = tok_rows // lax.axis_size("tp")
    tp_index = lax.axis_index("tp")
    all_heads = lax.all_gather(attended, "tp", axis=1, tiled=True)
    projected = jnp.dot(all_heads, out_weight, preferred_element_type=jnp.float32)
    stream = (residual.astype(jnp.float32) + projected).astype(jnp.bfloat16)
    normed = normalize(stream, norm_gain)
    stream_own = lax.dynamic_slice_in_dim(stream, tp_index * share, share, 0)
    pieces = (
        lax.all_gather(gate_weight, "sp", axis=0, tiled=True),
        lax.all_gather(value_weight, "sp", axis=0, tiled=True),
    )
    gate_sum = jnp.dot(normed, pieces[0], preferred_element_type=jnp.float32)
    value_sum = jnp.dot(normed, pieces[1], preferred_element_type=jnp.float32)
    gate_pre = gate_sum.astype(jnp.bfloat16)
    value_pre = value_sum.astype(jnp.bfloat16)
    reach = conv_weight.shape[0] // 2
    padded = padded_2(gate_pre, (("sp", 0),), reach)
    mixed_gate = jnp.zeros(gate_pre.shape, jnp.float32)
    for tap in range(conv_weight.shape[0]):
        mixed_gate = mixed_gate + padded[tap : tap + tok_rows].astype(jnp.float32) * conv_weight[
            tap
        ].astype(jnp.float32)
    active = (jax.nn.silu(mixed_gate) * value_pre.astype(jnp.float32)).astype(jnp.bfloat16)
    partial_rows = jnp.dot(
        active,
        lax.all_gather(down_weight, "sp", axis=1, tiled=True),
        preferred_element_type=jnp.float32,
    )
    summed = lax.psum_scatter(
        partial_rows.astype(jnp.bfloat16), "tp", scatter_dimension=0, tiled=True
    ).astype(jnp.float32)
    return (stream_own.astype(jnp.float32) + summed).astype(jnp.bfloat16)


MESH = pl.DeviceIdType.MESH


def layer_kernel(
    zn,
    table_ref,
    q_ref,
    lat_ref,
    key_ref,
    expand_ref,
    res_ref,
    out_w_ref,
    gain_ref,
    gate_ref,
    value_ref,
    conv_ref,
    down_ref,
    out_ref,
    lat_all,
    att_send,
    att_recv,
    nrm,
    stage,
    w_full,
    dn_full,
    hbuf,
    abuf,
    halo_send,
    halo_recv,
    part,
    c_send,
    c_recv,
    keep,
    x_send,
    x_recv,
    z_send,
    z_recv,
    lz_s, lz_r, ly_s, ly_r, lc_s, lc_r,
    wz_s, wz_r, wy_s, wy_r,
    dz_s, dz_r, dy_s, dy_r,
    at_s, at_r,
    nz_s, nz_r, nx_s, nx_r, nc_s, nc_r,
    h_s, h_r,
    pc_s, pc_r, px_s, px_r, pz_s, pz_r,
):
    f32, bf16 = jnp.float32, jnp.bfloat16
    s, t = lax.axis_index("sp"), lax.axis_index("tp")
    z, y = s // 2, s % 2
    x, c = t // 2, t % 2
    yo, xo, co = 1 - y, 1 - x, 1 - c
    rows = q_ref.shape[0]
    half, share = rows // 2, rows // 4
    rank = lat_ref.shape[1]
    sub = down_ref.shape[0] // zn
    sp = 2 * zn

    def to_z(d):
        return {"sp": 2 * ((z + d) % zn) + y, "tp": t}

    y_dev = {"sp": 2 * z + yo, "tp": t}
    x_dev = {"sp": s, "tp": 2 * xo + c}
    c_dev = {"sp": s, "tp": 2 * x + co}

    def from_z(d):
        return (z + zn - d) % zn

    started = []

    def send(src, dst, s_sem, r_sem, dev):
        copy = pltpu.make_async_remote_copy(
            src_ref=src, dst_ref=dst, send_sem=s_sem, recv_sem=r_sem,
            device_id=dev, device_id_type=MESH,
        )
        copy.start()
        started.append(copy)
        return copy

    def arrived(dst, s_sem, r_sem):
        pltpu.make_async_remote_copy(
            src_ref=dst, dst_ref=dst, send_sem=s_sem, recv_sem=r_sem,
            device_id=c_dev, device_id_type=MESH,
        ).wait_recv()

    barrier = pltpu.get_barrier_semaphore()
    partners = [to_z(d) for d in range(1, zn)] + [y_dev, x_dev, c_dev, {"sp": s, "tp": 2 * xo + co}]
    for dev in partners:
        pl.semaphore_signal(barrier, inc=1, device_id=dev, device_id_type=MESH)

    cos2 = table_ref[:, : 2 * (ROPE // 2)]
    sin2 = table_ref[:, ROPE : 2 * ROPE]

    def turn(v):
        v = v.astype(f32)
        h = ROPE // 2
        swapped = jnp.concatenate([v[:, h:], v[:, :h]], axis=1)
        return (v * cos2 + swapped * sin2).astype(bf16)

    key_turned = turn(key_ref[...])
    for i in range(2):
        lat_all[s, i, :, :rank] = lat_ref[i * half : (i + 1) * half, :]
        lat_all[s, i, :, rank : rank + ROPE] = key_turned[i * half : (i + 1) * half, :]
        lat_all[s, i, :, rank + ROPE :] = jnp.zeros((half, ROPE), bf16)
    pl.semaphore_wait(barrier, len(partners))

    mine = lat_all.at[s, c]
    for d in range(1, zn):
        send(mine, mine, lz_s.at[d], lz_r.at[d], to_z(d))
    send(mine, mine, ly_s.at[0], ly_r.at[0], y_dev)

    for k in range(zn):
        stage[k, :, :sub] = gate_ref[:, k * sub : (k + 1) * sub]
        stage[k, :, sub:] = value_ref[:, k * sub : (k + 1) * sub]

    for d in range(1, zn):
        blk = lat_all.at[2 * from_z(d) + y, c]
        arrived(blk, lz_s.at[d], lz_r.at[d])
        send(blk, blk, ly_s.at[d], ly_r.at[d], y_dev)
        send(blk, blk, lc_s.at[d], lc_r.at[d], c_dev)
    w_full[s] = stage[z]
    dn_full[s] = down_ref[pl.ds(pl.multiple_of(z * sub, sub), sub), :]
    for d in range(1, zn):
        zz = (z + d) % zn
        send(stage.at[zz], w_full.at[s], wz_s.at[d], wz_r.at[d], to_z(d))
        send(down_ref.at[pl.ds(pl.multiple_of(zz * sub, sub), sub), :], dn_full.at[s], dz_s.at[d], dz_r.at[d], to_z(d))
    for d in range(zn):
        blk = lat_all.at[2 * from_z(d) + yo, c]
        arrived(blk, ly_s.at[d], ly_r.at[d])
        send(blk, blk, lc_s.at[zn + d], lc_r.at[zn + d], c_dev)
    send(w_full.at[s], w_full.at[s], wy_s.at[0], wy_r.at[0], y_dev)
    send(dn_full.at[s], dn_full.at[s], dy_s.at[0], dy_r.at[0], y_dev)
    q_wide = q_ref[:, :NOPE_A]
    q_narrow = q_ref[:, NOPE_A : NOPE_A + NOPE_B]
    rot = NOPE_A + NOPE_B
    q_wide_t = turn(q_ref[:, rot : rot + ROPE])
    q_narrow_t = turn(q_ref[:, rot + ROPE : rot + 2 * ROPE])
    for d in range(1, zn):
        arrived(lat_all.at[2 * from_z(d) + y, co], lc_s.at[d], lc_r.at[d])
    for d in range(zn):
        arrived(lat_all.at[2 * from_z(d) + yo, co], lc_s.at[zn + d], lc_r.at[zn + d])

    whole = lat_all[...].reshape(sp * rows, lat_all.shape[3])
    expanded = jnp.dot(whole[:, :rank], expand_ref[...], preferred_element_type=f32).astype(bf16)
    keys_t = whole[:, rank : rank + ROPE]

    def attend(qc, qt, kc, v, scale):
        dims = (((1,), (1,)), ((), ()))
        scores = (
            lax.dot_general(qc, kc, dims, preferred_element_type=f32)
            + lax.dot_general(qt, keys_t, dims, preferred_element_type=f32)
        ) * scale
        w = jnp.exp(scores - jnp.max(scores, axis=1, keepdims=True))
        total = jnp.sum(w, axis=1, keepdims=True)
        return (jnp.dot(w.astype(bf16), v, preferred_element_type=f32) / total).astype(bf16)

    nb = NOPE_A + VAL_A
    wide = attend(q_wide, q_wide_t, expanded[:, :NOPE_A], expanded[:, NOPE_A:nb], (NOPE_A + ROPE) ** -0.5)
    narrow = attend(
        q_narrow, q_narrow_t, expanded[:, nb : nb + NOPE_B],
        expanded[:, nb + NOPE_B : nb + NOPE_B + VAL_B], (NOPE_B + ROPE) ** -0.5,
    )
    vals = VAL_A + VAL_B
    for i in range(4):
        att_send[i, :, :VAL_A] = wide[i * share : (i + 1) * share, :]
        att_send[i, :, VAL_A:vals] = narrow[i * share : (i + 1) * share, :]
    others = [(2 * x + co), (2 * xo + c), (2 * xo + co)]
    for i, o in enumerate(others):
        send(att_send.at[o], att_recv.at[t], at_s.at[i], at_r.at[i], {"sp": s, "tp": o})
    att_recv[t] = att_send[t]

    def forward_weights(d):
        blk = w_full.at[2 * from_z(d) + y]
        arrived(blk, wz_s.at[d], wz_r.at[d])
        send(blk, blk, wy_s.at[d], wy_r.at[d], y_dev)
        blk = dn_full.at[2 * from_z(d) + y]
        arrived(blk, dz_s.at[d], dz_r.at[d])
        send(blk, blk, dy_s.at[d], dy_r.at[d], y_dev)

    for i, o in enumerate(others):
        arrived(att_recv.at[o], at_s.at[i], at_r.at[i])
    projected = jnp.dot(att_recv[0, :, :vals], out_w_ref[:vals, :], preferred_element_type=f32)
    for i in range(1, 4):
        projected += jnp.dot(
            att_recv[i, :, :vals], out_w_ref[i * vals : (i + 1) * vals, :], preferred_element_type=f32
        )
    mine_rows = pl.ds(pl.multiple_of(t * share, share), share)
    stream = (res_ref[mine_rows, :].astype(f32) + projected).astype(bf16)
    stream_f = stream.astype(f32)
    scaled = stream_f * lax.rsqrt(jnp.mean(stream_f * stream_f, axis=1, keepdims=True) + 1e-06)
    nrm[z, t] = (scaled * gain_ref[...].astype(f32)).astype(bf16)

    own = nrm.at[z, t]
    for d in range(1, zn):
        send(own, own, nz_s.at[d], nz_r.at[d], to_z(d))
    send(own, own, nx_s.at[0], nx_r.at[0], x_dev)
    send(own, own, nc_s.at[0], nc_r.at[0], c_dev)
    forward_weights(1)
    xt = 2 * xo + c
    blk = nrm.at[z, xt]
    arrived(blk, nx_s.at[0], nx_r.at[0])
    send(blk, blk, nc_s.at[zn], nc_r.at[zn], c_dev)
    for d in range(1, zn):
        blk = nrm.at[from_z(d), t]
        arrived(blk, nz_s.at[d], nz_r.at[d])
        send(blk, blk, nx_s.at[d], nx_r.at[d], x_dev)
        send(blk, blk, nc_s.at[d], nc_r.at[d], c_dev)
        if d > 1:
            forward_weights(d)
    for d in range(1, zn):
        blk = nrm.at[from_z(d), xt]
        arrived(blk, nx_s.at[d], nx_r.at[d])
        send(blk, blk, nc_s.at[zn + d], nc_r.at[zn + d], c_dev)
    for d in range(zn):
        arrived(w_full.at[2 * from_z(d) + yo], wy_s.at[d], wy_r.at[d])
    weights = w_full[...].reshape(sp * w_full.shape[1], 2 * sub)
    for d in range(zn):
        zz = from_z(d)
        arrived(nrm.at[zz, 2 * x + co], nc_s.at[d], nc_r.at[d])
        arrived(nrm.at[zz, 2 * xo + co], nc_s.at[zn + d], nc_r.at[zn + d])
        block = nrm[zz].reshape(rows, nrm.shape[3])
        hbuf[zz] = jnp.dot(block, weights, preferred_element_type=f32).astype(bf16)

    wide_lanes = halo_send.shape[1]
    for k in range(zn):
        g = hbuf[k, :, :wide_lanes].astype(f32)
        halo_send[k : k + 1, :] = g[rows - 1 : rows, :]
        halo_send[zn + k : zn + k + 1, :] = g[0:1, :]
    send(halo_send, halo_recv, h_s.at[0], h_r.at[0], y_dev)
    taps = jnp.zeros((conv_ref.shape[0], wide_lanes), f32)
    conv_all = conv_ref[...].astype(f32)
    pieces = [conv_all[:, k * sub : (k + 1) * sub] for k in range(zn)]
    taps = pieces[0]
    for k in range(1, zn):
        taps = jnp.where(z == k, pieces[k], taps)
    taps = jnp.concatenate([taps, jnp.zeros((taps.shape[0], wide_lanes - sub), f32)], axis=1)
    row_id = lax.broadcasted_iota(jnp.int32, (rows, wide_lanes), 0)
    arrived(halo_recv, h_s.at[0], h_r.at[0])
    nothing = jnp.zeros((1, wide_lanes), f32)
    for k in range(zn):
        before_low = halo_recv[k - 1 : k, :] if k > 0 else nothing
        before = jnp.where(y == 0, before_low, halo_recv[k : k + 1, :])
        after_high = halo_recv[zn + k + 1 : zn + k + 2, :] if k < zn - 1 else nothing
        after = jnp.where(y == 0, halo_recv[zn + k : zn + k + 1, :], after_high)
        g = hbuf[k, :, :wide_lanes].astype(f32)
        up = jnp.where(row_id == 0, before, pltpu.roll(g, 1, 0))
        down = jnp.where(row_id == rows - 1, after, pltpu.roll(g, rows - 1, 0))
        mixed = up * taps[0:1] + g * taps[1:2] + down * taps[2:3]
        mixed = mixed[:, :sub]
        v = hbuf[k].astype(f32)[:, sub:]
        abuf[k] = (mixed / (1.0 + jnp.exp(-mixed)) * v).astype(bf16)

    for d in range(zn):
        arrived(dn_full.at[2 * from_z(d) + yo], dy_s.at[d], dy_r.at[d])
    order = list(range(1, zn)) + [0]
    depth = dn_full.shape[2]
    for d in order:
        zz = (z + d) % zn
        a = abuf[zz]
        for k in range(sp):
            p = jnp.dot(a, dn_full[k], preferred_element_type=f32)
            part[d, :, :, k * depth : (k + 1) * depth] = p.reshape(4, share, depth)
        for i in range(2):
            c_send[d, i] = part[d, 2 * i + co].astype(bf16)
        send(c_send.at[d], c_recv.at[d], pc_s.at[d], pc_r.at[d], c_dev)
    for d in order:
        arrived(c_recv.at[d], pc_s.at[d], pc_r.at[d])
        x_send[d] = (part[d, 2 * xo + c] + c_recv[d, xo].astype(f32)).astype(bf16)
        send(x_send.at[d], x_recv.at[d], px_s.at[d], px_r.at[d], x_dev)
        keep[d] = part[d, 2 * x + c] + c_recv[d, x].astype(f32)
    for d in order:
        arrived(x_recv.at[d], px_s.at[d], px_r.at[d])
        if d > 0:
            z_send[d] = (keep[d] + x_recv[d].astype(f32)).astype(bf16)
            send(z_send.at[d], z_recv.at[d], pz_s.at[d], pz_r.at[d], to_z(d))
    total = keep[0] + x_recv[0].astype(f32)
    for d in range(1, zn):
        arrived(z_recv.at[d], pz_s.at[d], pz_r.at[d])
        total += z_recv[d].astype(f32)
    out_ref[...] = (stream_f + total).astype(bf16)
    for copy in started:
        copy.wait_send()


def kernel_body(zn, *args):
    (queries, latents, shared_key, expand_weight, residual, out_weight, norm_gain,
     gate_weight, value_weight, conv_weight, down_weight) = args
    rows, width = residual.shape
    sub = down_weight.shape[0] // zn
    share, half = rows // 4, rows // 2
    d_own = gate_weight.shape[0]
    positions = lax.axis_index("sp") * rows + jnp.arange(rows, dtype=jnp.int32)
    cos_table, sine_table = tables(positions, ROPE)
    table = jnp.concatenate([cos_table, cos_table, -sine_table, sine_table], axis=1)
    bf16, f32 = jnp.bfloat16, jnp.float32
    vals = VAL_A + VAL_B
    lanes = -(-vals // 128) * 128
    halo_lanes = -(-sub // 128) * 128
    V, DMA = pltpu.VMEM, pltpu.SemaphoreType.DMA
    sems = []
    for count in (zn, zn, 2 * zn, zn, zn, zn, zn, 3, zn, zn, 2 * zn, 1, zn, zn, zn):
        sems += [DMA((count,)), DMA((count,))]
    return pl.pallas_call(
        functools.partial(layer_kernel, zn),
        out_shape=jax.ShapeDtypeStruct((share, width), bf16),
        in_specs=[pl.BlockSpec(memory_space=V)] * 12,
        out_specs=pl.BlockSpec(memory_space=V),
        scratch_shapes=[
            V((2 * zn, 2, half, latents.shape[1] + 2 * ROPE), bf16),
            V((4, share, lanes), bf16),
            V((4, share, lanes), bf16),
            V((zn, 4, share, width), bf16),
            V((zn, d_own, 2 * sub), bf16),
            V((2 * zn, d_own, 2 * sub), bf16),
            V((2 * zn, sub, down_weight.shape[1]), bf16),
            V((zn, rows, 2 * sub), bf16),
            V((zn, rows, sub), bf16),
            V((2 * zn, halo_lanes), f32),
            V((2 * zn, halo_lanes), f32),
            V((zn, 4, share, width), f32),
            V((zn, 2, share, width), bf16),
            V((zn, 2, share, width), bf16),
            V((zn, share, width), f32),
            V((zn, share, width), bf16),
            V((zn, share, width), bf16),
            V((zn, share, width), bf16),
            V((zn, share, width), bf16),
        ] + sems,
        compiler_params=pltpu.CompilerParams(collective_id=0, has_side_effects=True),
    )(table, queries, latents, shared_key, expand_weight, residual, out_weight,
      norm_gain.reshape(1, -1), gate_weight, value_weight, conv_weight, down_weight)


def pick(*args):
    zn = lax.axis_size("sp") // 2
    hidden = args[10].shape[0]
    sub = hidden // zn
    fits = (
        lax.axis_size("sp") % 2 == 0
        and lax.axis_size("tp") == 4
        and hidden % zn == 0
        and sub % 64 == 0
        and args[7].shape[0] % 128 == 0
        and args[0].shape[0] % 64 == 0
        and args[9].shape[0] == 3
    )
    return kernel_body(zn, *args) if fits else body(*args)


def solution(mesh):
    in_specs = (
        P("sp", "tp"),
        P("sp", None),
        P("sp", None),
        P(None, "tp"),
        P("sp", None),
        P(),
        P(),
        P("sp", "tp"),
        P("sp", "tp"),
        P(None, "tp"),
        P("tp", "sp"),
    )
    out_specs = P(("sp", "tp"), None)
    return jax.shard_map(pick, mesh=mesh, in_specs=in_specs, out_specs=out_specs, check_vma=False)
```

```python
import functools

import jax
import jax.numpy as jnp
from jax import lax
from jax.experimental import pallas as pl
from jax.experimental.pallas import tpu as pltpu
from jax.sharding import PartitionSpec as P

NOPE_A = 128
VAL_A = 128
NOPE_B = 64
VAL_B = 64
ROPE = 64


def padded_2(block, sides, width):
    for axis, dim in sides:
        count = lax.axis_size(axis)
        forward = [(i, i + 1) for i in range(count - 1)]
        backward = [(target, source) for source, target in forward]
        low = lax.ppermute(
            lax.slice_in_dim(block, block.shape[dim] - width, None, axis=dim), axis, forward
        )
        high = lax.ppermute(lax.slice_in_dim(block, 0, width, axis=dim), axis, backward)
        block = jnp.concatenate([low, block, high], axis=dim)
    return block


def tables(positions, width):
    half_width = width // 2
    frequency = 10000.0 ** (-jnp.arange(half_width, dtype=jnp.float32) / half_width)
    angles = positions.astype(jnp.float32)[:, None] * frequency[None, :]
    return (jnp.cos(angles), jnp.sin(angles))


def rotate(vectors, cos_table, sine_table):
    half_width = vectors.shape[-1] // 2
    first_half = vectors[:, :half_width].astype(jnp.float32)
    second_half = vectors[:, half_width:].astype(jnp.float32)
    turned = jnp.concatenate(
        [
            first_half * cos_table - second_half * sine_table,
            second_half * cos_table + first_half * sine_table,
        ],
        axis=1,
    )
    return turned.astype(jnp.bfloat16)


def normalize(stream, norm_gain):
    stream_f = stream.astype(jnp.float32)
    scaled = stream_f * lax.rsqrt(jnp.mean(stream_f * stream_f, axis=1, keepdims=True) + 1e-06)
    return (scaled * norm_gain.astype(jnp.float32)).astype(jnp.bfloat16)


def update(running, q_content, q_turned, k_content, k_turned, values, score_scale):
    row_max, row_sum, weighted = running
    scores = (
        jnp.einsum("qd,kd->qk", q_content, k_content, preferred_element_type=jnp.float32)
        + jnp.einsum("qd,kd->qk", q_turned, k_turned, preferred_element_type=jnp.float32)
    ) * score_scale
    new_max = jnp.maximum(row_max, jnp.max(scores, axis=1))
    weights = jnp.exp(scores - new_max[:, None])
    row_sum = jnp.sum(weights, axis=1)
    weighted = jnp.dot(weights.astype(jnp.bfloat16), values, preferred_element_type=jnp.float32)
    return (new_max, row_sum, weighted)


def body(
    queries,
    latents,
    shared_key,
    expand_weight,
    residual,
    out_weight,
    norm_gain,
    gate_weight,
    value_weight,
    conv_weight,
    down_weight,
):
    tok_rows = queries.shape[0]
    q_width = NOPE_A + NOPE_B + 2 * ROPE
    kv_width = NOPE_A + VAL_A + NOPE_B + VAL_B
    positions = lax.axis_index("sp") * tok_rows + jnp.arange(tok_rows, dtype=jnp.int32)
    cos_table, sine_table = tables(positions, ROPE)
    key_turned = rotate(shared_key, cos_table, sine_table)
    scale_wide = (NOPE_A + ROPE) ** (-0.5)
    scale_narrow = (NOPE_B + ROPE) ** (-0.5)
    initial = []
    pair_index = 0
    q_base = pair_index * q_width
    rotary_base = q_base + NOPE_A + NOPE_B
    wide_content = queries[:, q_base : q_base + NOPE_A]
    narrow_content = queries[:, q_base + NOPE_A : rotary_base]
    wide_turned = rotate(queries[:, rotary_base : rotary_base + ROPE], cos_table, sine_table)
    narrow_turned = rotate(
        queries[:, rotary_base + ROPE : rotary_base + 2 * ROPE], cos_table, sine_table
    )
    query_parts = [(wide_content, wide_turned, narrow_content, narrow_turned)]
    lowest = jnp.full((tok_rows,), -1e30, jnp.float32)
    empty_sum = jnp.zeros((tok_rows,), jnp.float32)
    initial += [
        lowest,
        empty_sum,
        jnp.zeros((tok_rows, VAL_A), jnp.float32),
        lowest,
        empty_sum,
        jnp.zeros((tok_rows, VAL_B), jnp.float32),
    ]
    initial = tuple(initial)
    pieces = (
        lax.all_gather(latents, "sp", axis=0, tiled=True),
        lax.all_gather(key_turned, "sp", axis=0, tiled=True),
    )
    expanded = jnp.dot(pieces[0], expand_weight, preferred_element_type=jnp.float32).astype(
        jnp.bfloat16
    )
    turned_keys = pieces[1]
    result = []
    pair_index = 0
    wide_content, wide_turned, narrow_content, narrow_turned = query_parts[pair_index]
    kv_base = pair_index * kv_width
    narrow_base = kv_base + NOPE_A + VAL_A
    wide_keys = expanded[:, kv_base : kv_base + NOPE_A]
    wide_values = expanded[:, kv_base + NOPE_A : narrow_base]
    narrow_keys = expanded[:, narrow_base : narrow_base + NOPE_B]
    narrow_values = expanded[:, narrow_base + NOPE_B : narrow_base + NOPE_B + VAL_B]
    absorb_offset = 6 * pair_index
    result += list(
        update(
            initial[absorb_offset : absorb_offset + 3],
            wide_content,
            wide_turned,
            wide_keys,
            turned_keys,
            wide_values,
            scale_wide,
        )
    )
    result += list(
        update(
            initial[absorb_offset + 3 : absorb_offset + 6],
            narrow_content,
            narrow_turned,
            narrow_keys,
            turned_keys,
            narrow_values,
            scale_narrow,
        )
    )
    running = tuple(result)
    outputs = []
    pair_index = 0
    for group_index in range(2):
        offset = 6 * pair_index + 3 * group_index
        outputs.append((running[offset + 2] / running[offset + 1][:, None]).astype(jnp.bfloat16))
    attended = jnp.concatenate(outputs, axis=1)
    share = tok_rows // lax.axis_size("tp")
    tp_index = lax.axis_index("tp")
    all_heads = lax.all_gather(attended, "tp", axis=1, tiled=True)
    projected = jnp.dot(all_heads, out_weight, preferred_element_type=jnp.float32)
    stream = (residual.astype(jnp.float32) + projected).astype(jnp.bfloat16)
    normed = normalize(stream, norm_gain)
    stream_own = lax.dynamic_slice_in_dim(stream, tp_index * share, share, 0)
    pieces = (
        lax.all_gather(gate_weight, "sp", axis=0, tiled=True),
        lax.all_gather(value_weight, "sp", axis=0, tiled=True),
    )
    gate_sum = jnp.dot(normed, pieces[0], preferred_element_type=jnp.float32)
    value_sum = jnp.dot(normed, pieces[1], preferred_element_type=jnp.float32)
    gate_pre = gate_sum.astype(jnp.bfloat16)
    value_pre = value_sum.astype(jnp.bfloat16)
    reach = conv_weight.shape[0] // 2
    padded = padded_2(gate_pre, (("sp", 0),), reach)
    mixed_gate = jnp.zeros(gate_pre.shape, jnp.float32)
    for tap in range(conv_weight.shape[0]):
        mixed_gate = mixed_gate + padded[tap : tap + tok_rows].astype(jnp.float32) * conv_weight[
            tap
        ].astype(jnp.float32)
    active = (jax.nn.silu(mixed_gate) * value_pre.astype(jnp.float32)).astype(jnp.bfloat16)
    partial_rows = jnp.dot(
        active,
        lax.all_gather(down_weight, "sp", axis=1, tiled=True),
        preferred_element_type=jnp.float32,
    )
    summed = lax.psum_scatter(
        partial_rows.astype(jnp.bfloat16), "tp", scatter_dimension=0, tiled=True
    ).astype(jnp.float32)
    return (stream_own.astype(jnp.float32) + summed).astype(jnp.bfloat16)


MESH = pl.DeviceIdType.MESH


def layer_kernel(
    zn,
    table_ref,
    q_ref,
    lat_ref,
    key_ref,
    conv_ref,
    expand_hbm,
    res_hbm,
    out_w_hbm,
    gate_hbm,
    value_hbm,
    down_hbm,
    out_ref,
    expand_ref,
    res_ref,
    out_w_ref,
    gate_ref,
    value_ref,
    down_ref,
    lat_all,
    att_send,
    att_recv,
    nrm,
    stage,
    w_full,
    dn_full,
    hbuf,
    abuf,
    halo_send,
    halo_recv,
    part,
    c_send,
    c_recv,
    keep,
    x_send,
    x_recv,
    z_send,
    z_recv,
    in_s,
    lz_s, lz_r, ly_s, ly_r, lc_s, lc_r,
    wz_s, wz_r, wy_s, wy_r,
    dz_s, dz_r, dy_s, dy_r,
    at_s, at_r,
    nz_s, nz_r, nx_s, nx_r, nc_s, nc_r,
    h_s, h_r,
    pc_s, pc_r, px_s, px_r, pz_s, pz_r,
):
    f32, bf16 = jnp.float32, jnp.bfloat16
    s, t = lax.axis_index("sp"), lax.axis_index("tp")
    z, y = s // 2, s % 2
    x, c = t // 2, t % 2
    yo, xo, co = 1 - y, 1 - x, 1 - c
    rows = lat_ref.shape[0]
    half, share = rows // 2, rows // 4
    rank = lat_ref.shape[1]
    sub = down_ref.shape[0] // zn
    sp = 2 * zn

    def to_z(d):
        return {"sp": 2 * ((z + d) % zn) + y, "tp": t}

    y_dev = {"sp": 2 * z + yo, "tp": t}
    x_dev = {"sp": s, "tp": 2 * xo + c}
    c_dev = {"sp": s, "tp": 2 * x + co}

    def from_z(d):
        return (z + zn - d) % zn

    started = []

    def send(src, dst, s_sem, r_sem, dev):
        copy = pltpu.make_async_remote_copy(
            src_ref=src, dst_ref=dst, send_sem=s_sem, recv_sem=r_sem,
            device_id=dev, device_id_type=MESH,
        )
        copy.start()
        started.append(copy)
        return copy

    def arrived(dst, s_sem, r_sem):
        pltpu.make_async_remote_copy(
            src_ref=dst, dst_ref=dst, send_sem=s_sem, recv_sem=r_sem,
            device_id=c_dev, device_id_type=MESH,
        ).wait_recv()

    barrier = pltpu.get_barrier_semaphore()
    partners = [to_z(d) for d in range(1, zn)] + [y_dev, x_dev, c_dev, {"sp": s, "tp": 2 * xo + co}]
    for dev in partners:
        pl.semaphore_signal(barrier, inc=1, device_id=dev, device_id_type=MESH)

    mine_rows = pl.ds(pl.multiple_of(t * share, share), share)
    loads = [
        pltpu.make_async_copy(src, dst, in_s.at[i])
        for i, (src, dst) in enumerate(
            [
                (gate_hbm, gate_ref),
                (value_hbm, value_ref),
                (down_hbm, down_ref),
                (expand_hbm, expand_ref),
                (res_hbm.at[mine_rows, :], res_ref),
                (out_w_hbm, out_w_ref),
            ]
        )
    ]
    for load in loads:
        load.start()

    h = ROPE // 2
    cos, sine = table_ref[:h, :], table_ref[h:ROPE, :]

    def turn(v):
        a, b = v[:h], v[h:]
        return jnp.concatenate([a * cos - b * sine, b * cos + a * sine], axis=0)

    rot = NOPE_A + NOPE_B
    q = q_ref[...].astype(f32)
    pair = jnp.concatenate([turn(q[rot + ROPE :]), turn(key_ref[...].astype(f32))], axis=0).T.astype(bf16)
    q_narrow_t, key_turned = pair[:, :ROPE], pair[:, ROPE:]
    for i in range(2):
        lat_all[s, i, :, :rank] = lat_ref[i * half : (i + 1) * half, :]
        lat_all[s, i, :, rank : rank + ROPE] = key_turned[i * half : (i + 1) * half, :]
        lat_all[s, i, :, rank + ROPE :] = jnp.zeros((half, ROPE), bf16)
    pl.semaphore_wait(barrier, len(partners))

    mine = lat_all.at[s, c]
    for d in range(1, zn):
        send(mine, mine, lz_s.at[d], lz_r.at[d], to_z(d))
    send(mine, mine, ly_s.at[0], ly_r.at[0], y_dev)

    loads[0].wait()
    loads[1].wait()
    for k in range(zn):
        stage[k, :, :sub] = gate_ref[:, k * sub : (k + 1) * sub]
        stage[k, :, sub:] = value_ref[:, k * sub : (k + 1) * sub]
    for d in range(1, zn):
        send(stage.at[(z + d) % zn], w_full.at[s], wz_s.at[d], wz_r.at[d], to_z(d))
    w_full[s] = stage[z]
    loads[2].wait()

    def send_down(d):
        zz = (z + d) % zn
        piece = down_ref.at[pl.ds(pl.multiple_of(zz * sub, sub), sub), :]
        send(piece, dn_full.at[s], dz_s.at[d], dz_r.at[d], to_z(d))

    send_down(1)
    dn_full[s] = down_ref[pl.ds(pl.multiple_of(z * sub, sub), sub), :]

    for d in range(1, zn):
        blk = lat_all.at[2 * from_z(d) + y, c]
        arrived(blk, lz_s.at[d], lz_r.at[d])
        send(blk, blk, ly_s.at[d], ly_r.at[d], y_dev)
        send(blk, blk, lc_s.at[d], lc_r.at[d], c_dev)
    send(w_full.at[s], w_full.at[s], wy_s.at[0], wy_r.at[0], y_dev)
    for d in range(zn):
        blk = lat_all.at[2 * from_z(d) + yo, c]
        arrived(blk, ly_s.at[d], ly_r.at[d])
        send(blk, blk, lc_s.at[zn + d], lc_r.at[zn + d], c_dev)
    q_wide = q[:NOPE_A].T.astype(bf16)
    pair = jnp.concatenate([q[NOPE_A:rot], turn(q[rot : rot + ROPE])], axis=0).T.astype(bf16)
    q_narrow, q_wide_t = pair[:, :NOPE_B], pair[:, NOPE_B:]
    loads[3].wait()
    for d in range(1, zn):
        arrived(lat_all.at[2 * from_z(d) + y, co], lc_s.at[d], lc_r.at[d])
    for d in range(zn):
        arrived(lat_all.at[2 * from_z(d) + yo, co], lc_s.at[zn + d], lc_r.at[zn + d])

    whole = lat_all[...].reshape(sp * rows, lat_all.shape[3])
    expanded = jnp.dot(whole[:, :rank], expand_ref[...], preferred_element_type=f32).astype(bf16)
    keys_t = whole[:, rank : rank + ROPE]

    def attend(qc, qt, kc, v, scale):
        dims = (((1,), (1,)), ((), ()))
        scores = (
            lax.dot_general(qc, kc, dims, preferred_element_type=f32)
            + lax.dot_general(qt, keys_t, dims, preferred_element_type=f32)
        ) * scale
        w = jnp.exp(scores - jnp.max(scores, axis=1, keepdims=True))
        total = jnp.sum(w, axis=1, keepdims=True)
        return (jnp.dot(w.astype(bf16), v, preferred_element_type=f32) / total).astype(bf16)

    nb = NOPE_A + VAL_A
    wide = attend(q_wide, q_wide_t, expanded[:, :NOPE_A], expanded[:, NOPE_A:nb], (NOPE_A + ROPE) ** -0.5)
    narrow = attend(
        q_narrow, q_narrow_t, expanded[:, nb : nb + NOPE_B],
        expanded[:, nb + NOPE_B : nb + NOPE_B + VAL_B], (NOPE_B + ROPE) ** -0.5,
    )
    vals = VAL_A + VAL_B
    for i in range(4):
        att_send[i, :, :VAL_A] = wide[i * share : (i + 1) * share, :]
        att_send[i, :, VAL_A:vals] = narrow[i * share : (i + 1) * share, :]
    others = [(2 * x + co), (2 * xo + c), (2 * xo + co)]
    for i, o in enumerate(others):
        send(att_send.at[o], att_recv.at[t], at_s.at[i], at_r.at[i], {"sp": s, "tp": o})
    att_recv[t] = att_send[t]

    def forward(full, sz, rz, sy, ry, d):
        blk = full.at[2 * from_z(d) + y]
        arrived(blk, sz.at[d], rz.at[d])
        send(blk, blk, sy.at[d], ry.at[d], y_dev)

    def forward_weights(d):
        forward(w_full, wz_s, wz_r, wy_s, wy_r, d)

    loads[4].wait()
    loads[5].wait()
    for i, o in enumerate(others):
        arrived(att_recv.at[o], at_s.at[i], at_r.at[i])
    projected = jnp.dot(att_recv[0, :, :vals], out_w_ref[:vals, :], preferred_element_type=f32)
    for i in range(1, 4):
        projected += jnp.dot(
            att_recv[i, :, :vals], out_w_ref[i * vals : (i + 1) * vals, :], preferred_element_type=f32
        )
    stream = (res_ref[...].astype(f32) + projected).astype(bf16)
    stream_f = stream.astype(f32)
    scaled = stream_f * lax.rsqrt(jnp.mean(stream_f * stream_f, axis=1, keepdims=True) + 1e-06)
    for k in range(scaled.shape[1] // rows):
        gain = table_ref[ROPE + k : ROPE + k + 1, :]
        nrm[z, t, :, k * rows : (k + 1) * rows] = (scaled[:, k * rows : (k + 1) * rows] * gain).astype(bf16)

    own = nrm.at[z, t]
    for d in range(1, zn):
        send(own, own, nz_s.at[d], nz_r.at[d], to_z(d))
    send(own, own, nx_s.at[0], nx_r.at[0], x_dev)
    send(own, own, nc_s.at[0], nc_r.at[0], c_dev)
    for d in range(2, zn):
        send_down(d)
    forward_weights(1)
    xt = 2 * xo + c
    blk = nrm.at[z, xt]
    arrived(blk, nx_s.at[0], nx_r.at[0])
    send(blk, blk, nc_s.at[zn], nc_r.at[zn], c_dev)
    for d in range(1, zn):
        blk = nrm.at[from_z(d), t]
        arrived(blk, nz_s.at[d], nz_r.at[d])
        send(blk, blk, nx_s.at[d], nx_r.at[d], x_dev)
        send(blk, blk, nc_s.at[d], nc_r.at[d], c_dev)
        if d > 1:
            forward_weights(d)
    for d in range(1, zn):
        blk = nrm.at[from_z(d), xt]
        arrived(blk, nx_s.at[d], nx_r.at[d])
        send(blk, blk, nc_s.at[zn + d], nc_r.at[zn + d], c_dev)
    send(dn_full.at[s], dn_full.at[s], dy_s.at[0], dy_r.at[0], y_dev)
    forward(dn_full, dz_s, dz_r, dy_s, dy_r, 1)
    for d in range(zn):
        arrived(w_full.at[2 * from_z(d) + yo], wy_s.at[d], wy_r.at[d])
    weights = w_full[...].reshape(sp * w_full.shape[1], 2 * sub)
    for d in range(zn):
        zz = from_z(d)
        arrived(nrm.at[zz, 2 * x + co], nc_s.at[d], nc_r.at[d])
        arrived(nrm.at[zz, 2 * xo + co], nc_s.at[zn + d], nc_r.at[zn + d])
        block = nrm[zz].reshape(rows, nrm.shape[3])
        hbuf[zz] = jnp.dot(block, weights, preferred_element_type=f32).astype(bf16)

    for d in range(2, zn):
        forward(dn_full, dz_s, dz_r, dy_s, dy_r, d)
    wide_lanes = halo_send.shape[1]
    for k in range(zn):
        g = hbuf[k, :, :wide_lanes].astype(f32)
        halo_send[k : k + 1, :] = g[rows - 1 : rows, :]
        halo_send[zn + k : zn + k + 1, :] = g[0:1, :]
    send(halo_send, halo_recv, h_s.at[0], h_r.at[0], y_dev)
    taps = jnp.zeros((conv_ref.shape[0], wide_lanes), f32)
    conv_all = conv_ref[...].astype(f32)
    pieces = [conv_all[:, k * sub : (k + 1) * sub] for k in range(zn)]
    taps = pieces[0]
    for k in range(1, zn):
        taps = jnp.where(z == k, pieces[k], taps)
    taps = jnp.concatenate([taps, jnp.zeros((taps.shape[0], wide_lanes - sub), f32)], axis=1)
    row_id = lax.broadcasted_iota(jnp.int32, (rows, wide_lanes), 0)
    arrived(halo_recv, h_s.at[0], h_r.at[0])
    nothing = jnp.zeros((1, wide_lanes), f32)
    for k in range(zn):
        before_low = halo_recv[k - 1 : k, :] if k > 0 else nothing
        before = jnp.where(y == 0, before_low, halo_recv[k : k + 1, :])
        after_high = halo_recv[zn + k + 1 : zn + k + 2, :] if k < zn - 1 else nothing
        after = jnp.where(y == 0, halo_recv[zn + k : zn + k + 1, :], after_high)
        g = hbuf[k, :, :wide_lanes].astype(f32)
        up = jnp.where(row_id == 0, before, pltpu.roll(g, 1, 0))
        down = jnp.where(row_id == rows - 1, after, pltpu.roll(g, rows - 1, 0))
        mixed = up * taps[0:1] + g * taps[1:2] + down * taps[2:3]
        mixed = mixed[:, :sub]
        v = hbuf[k].astype(f32)[:, sub:]
        abuf[k] = (mixed / (1.0 + jnp.exp(-mixed)) * v).astype(bf16)

    for d in range(zn):
        arrived(dn_full.at[2 * from_z(d) + yo], dy_s.at[d], dy_r.at[d])
    order = list(range(1, zn)) + [0]
    depth = dn_full.shape[2]
    for d in order:
        zz = (z + d) % zn
        a = abuf[zz]
        for k in range(sp):
            p = jnp.dot(a, dn_full[k], preferred_element_type=f32)
            part[d, :, :, k * depth : (k + 1) * depth] = p.reshape(4, share, depth)
        for i in range(2):
            c_send[d, i] = part[d, 2 * i + co].astype(bf16)
        send(c_send.at[d], c_recv.at[d], pc_s.at[d], pc_r.at[d], c_dev)
    for d in order:
        arrived(c_recv.at[d], pc_s.at[d], pc_r.at[d])
        x_send[d] = (part[d, 2 * xo + c] + c_recv[d, xo].astype(f32)).astype(bf16)
        send(x_send.at[d], x_recv.at[d], px_s.at[d], px_r.at[d], x_dev)
        keep[d] = part[d, 2 * x + c] + c_recv[d, x].astype(f32)
    for d in order:
        arrived(x_recv.at[d], px_s.at[d], px_r.at[d])
        if d > 0:
            z_send[d] = (keep[d] + x_recv[d].astype(f32)).astype(bf16)
            send(z_send.at[d], z_recv.at[d], pz_s.at[d], pz_r.at[d], to_z(d))
    total = keep[0] + x_recv[0].astype(f32)
    for d in range(1, zn):
        arrived(z_recv.at[d], pz_s.at[d], pz_r.at[d])
        total += z_recv[d].astype(f32)
    out_ref[...] = (stream_f + total).astype(bf16)
    for copy in started:
        copy.wait_send()


def kernel_body(zn, *args):
    (queries, latents, shared_key, expand_weight, residual, out_weight, norm_gain,
     gate_weight, value_weight, conv_weight, down_weight) = args
    rows, width = residual.shape
    sub = down_weight.shape[0] // zn
    share, half = rows // 4, rows // 2
    d_own = gate_weight.shape[0]
    positions = lax.axis_index("sp") * rows + jnp.arange(rows, dtype=jnp.int32)
    cos_table, sine_table = tables(positions, ROPE)
    gain = norm_gain.reshape(width // rows, rows).astype(jnp.float32)
    table = jnp.concatenate([cos_table.T, sine_table.T, gain], axis=0)
    bf16, f32 = jnp.bfloat16, jnp.float32
    vals = VAL_A + VAL_B
    lanes = -(-vals // 128) * 128
    halo_lanes = -(-sub // 128) * 128
    V, DMA = pltpu.VMEM, pltpu.SemaphoreType.DMA
    sems = [DMA((6,))]
    for count in (zn, zn, 2 * zn, zn, zn, zn, zn, 3, zn, zn, 2 * zn, 1, zn, zn, zn):
        sems += [DMA((count,)), DMA((count,))]
    return pl.pallas_call(
        functools.partial(layer_kernel, zn),
        out_shape=jax.ShapeDtypeStruct((share, width), bf16),
        in_specs=[pl.BlockSpec(memory_space=V)] * 5 + [pl.BlockSpec(memory_space=pl.ANY)] * 6,
        out_specs=pl.BlockSpec(memory_space=V),
        scratch_shapes=[
            V(expand_weight.shape, bf16),
            V((share, width), bf16),
            V(out_weight.shape, bf16),
            V(gate_weight.shape, bf16),
            V(value_weight.shape, bf16),
            V(down_weight.shape, bf16),
            V((2 * zn, 2, half, latents.shape[1] + 2 * ROPE), bf16),
            V((4, share, lanes), bf16),
            V((4, share, lanes), bf16),
            V((zn, 4, share, width), bf16),
            V((zn, d_own, 2 * sub), bf16),
            V((2 * zn, d_own, 2 * sub), bf16),
            V((2 * zn, sub, down_weight.shape[1]), bf16),
            V((zn, rows, 2 * sub), bf16),
            V((zn, rows, sub), bf16),
            V((2 * zn, halo_lanes), f32),
            V((2 * zn, halo_lanes), f32),
            V((zn, 4, share, width), f32),
            V((zn, 2, share, width), bf16),
            V((zn, 2, share, width), bf16),
            V((zn, share, width), f32),
            V((zn, share, width), bf16),
            V((zn, share, width), bf16),
            V((zn, share, width), bf16),
            V((zn, share, width), bf16),
        ] + sems,
        compiler_params=pltpu.CompilerParams(collective_id=0, has_side_effects=True),
    )(table, queries.T, latents, shared_key.T, conv_weight, expand_weight, residual, out_weight,
      gate_weight, value_weight, down_weight)


def pick(*args):
    zn = lax.axis_size("sp") // 2
    hidden = args[10].shape[0]
    sub = hidden // zn
    fits = (
        lax.axis_size("sp") % 2 == 0
        and lax.axis_size("tp") == 4
        and hidden % zn == 0
        and sub % 64 == 0
        and args[7].shape[0] % 128 == 0
        and args[0].shape[0] % 128 == 0
        and args[4].shape[1] % args[0].shape[0] == 0
        and args[9].shape[0] == 3
    )
    return kernel_body(zn, *args) if fits else body(*args)


def solution(mesh):
    in_specs = (
        P("sp", "tp"),
        P("sp", None),
        P("sp", None),
        P(None, "tp"),
        P("sp", None),
        P(),
        P(),
        P("sp", "tp"),
        P("sp", "tp"),
        P(None, "tp"),
        P("tp", "sp"),
    )
    out_specs = P(("sp", "tp"), None)
    return jax.shard_map(pick, mesh=mesh, in_specs=in_specs, out_specs=out_specs, check_vma=False)
```

```python
import functools

import jax
import jax.numpy as jnp
from jax import lax
from jax.experimental import pallas as pl
from jax.experimental.pallas import tpu as pltpu
from jax.sharding import PartitionSpec as P

NOPE_A = 128
VAL_A = 128
NOPE_B = 64
VAL_B = 64
ROPE = 64


def padded_2(block, sides, width):
    for axis, dim in sides:
        count = lax.axis_size(axis)
        forward = [(i, i + 1) for i in range(count - 1)]
        backward = [(target, source) for source, target in forward]
        low = lax.ppermute(
            lax.slice_in_dim(block, block.shape[dim] - width, None, axis=dim), axis, forward
        )
        high = lax.ppermute(lax.slice_in_dim(block, 0, width, axis=dim), axis, backward)
        block = jnp.concatenate([low, block, high], axis=dim)
    return block


def tables(positions, width):
    half_width = width // 2
    frequency = 10000.0 ** (-jnp.arange(half_width, dtype=jnp.float32) / half_width)
    angles = positions.astype(jnp.float32)[:, None] * frequency[None, :]
    return (jnp.cos(angles), jnp.sin(angles))


def rotate(vectors, cos_table, sine_table):
    half_width = vectors.shape[-1] // 2
    first_half = vectors[:, :half_width].astype(jnp.float32)
    second_half = vectors[:, half_width:].astype(jnp.float32)
    turned = jnp.concatenate(
        [
            first_half * cos_table - second_half * sine_table,
            second_half * cos_table + first_half * sine_table,
        ],
        axis=1,
    )
    return turned.astype(jnp.bfloat16)


def normalize(stream, norm_gain):
    stream_f = stream.astype(jnp.float32)
    scaled = stream_f * lax.rsqrt(jnp.mean(stream_f * stream_f, axis=1, keepdims=True) + 1e-06)
    return (scaled * norm_gain.astype(jnp.float32)).astype(jnp.bfloat16)


def update(running, q_content, q_turned, k_content, k_turned, values, score_scale):
    row_max, row_sum, weighted = running
    scores = (
        jnp.einsum("qd,kd->qk", q_content, k_content, preferred_element_type=jnp.float32)
        + jnp.einsum("qd,kd->qk", q_turned, k_turned, preferred_element_type=jnp.float32)
    ) * score_scale
    new_max = jnp.maximum(row_max, jnp.max(scores, axis=1))
    weights = jnp.exp(scores - new_max[:, None])
    row_sum = jnp.sum(weights, axis=1)
    weighted = jnp.dot(weights.astype(jnp.bfloat16), values, preferred_element_type=jnp.float32)
    return (new_max, row_sum, weighted)


def body(
    queries,
    latents,
    shared_key,
    expand_weight,
    residual,
    out_weight,
    norm_gain,
    gate_weight,
    value_weight,
    conv_weight,
    down_weight,
):
    tok_rows = queries.shape[0]
    q_width = NOPE_A + NOPE_B + 2 * ROPE
    kv_width = NOPE_A + VAL_A + NOPE_B + VAL_B
    positions = lax.axis_index("sp") * tok_rows + jnp.arange(tok_rows, dtype=jnp.int32)
    cos_table, sine_table = tables(positions, ROPE)
    key_turned = rotate(shared_key, cos_table, sine_table)
    scale_wide = (NOPE_A + ROPE) ** (-0.5)
    scale_narrow = (NOPE_B + ROPE) ** (-0.5)
    initial = []
    pair_index = 0
    q_base = pair_index * q_width
    rotary_base = q_base + NOPE_A + NOPE_B
    wide_content = queries[:, q_base : q_base + NOPE_A]
    narrow_content = queries[:, q_base + NOPE_A : rotary_base]
    wide_turned = rotate(queries[:, rotary_base : rotary_base + ROPE], cos_table, sine_table)
    narrow_turned = rotate(
        queries[:, rotary_base + ROPE : rotary_base + 2 * ROPE], cos_table, sine_table
    )
    query_parts = [(wide_content, wide_turned, narrow_content, narrow_turned)]
    lowest = jnp.full((tok_rows,), -1e30, jnp.float32)
    empty_sum = jnp.zeros((tok_rows,), jnp.float32)
    initial += [
        lowest,
        empty_sum,
        jnp.zeros((tok_rows, VAL_A), jnp.float32),
        lowest,
        empty_sum,
        jnp.zeros((tok_rows, VAL_B), jnp.float32),
    ]
    initial = tuple(initial)
    pieces = (
        lax.all_gather(latents, "sp", axis=0, tiled=True),
        lax.all_gather(key_turned, "sp", axis=0, tiled=True),
    )
    expanded = jnp.dot(pieces[0], expand_weight, preferred_element_type=jnp.float32).astype(
        jnp.bfloat16
    )
    turned_keys = pieces[1]
    result = []
    pair_index = 0
    wide_content, wide_turned, narrow_content, narrow_turned = query_parts[pair_index]
    kv_base = pair_index * kv_width
    narrow_base = kv_base + NOPE_A + VAL_A
    wide_keys = expanded[:, kv_base : kv_base + NOPE_A]
    wide_values = expanded[:, kv_base + NOPE_A : narrow_base]
    narrow_keys = expanded[:, narrow_base : narrow_base + NOPE_B]
    narrow_values = expanded[:, narrow_base + NOPE_B : narrow_base + NOPE_B + VAL_B]
    absorb_offset = 6 * pair_index
    result += list(
        update(
            initial[absorb_offset : absorb_offset + 3],
            wide_content,
            wide_turned,
            wide_keys,
            turned_keys,
            wide_values,
            scale_wide,
        )
    )
    result += list(
        update(
            initial[absorb_offset + 3 : absorb_offset + 6],
            narrow_content,
            narrow_turned,
            narrow_keys,
            turned_keys,
            narrow_values,
            scale_narrow,
        )
    )
    running = tuple(result)
    outputs = []
    pair_index = 0
    for group_index in range(2):
        offset = 6 * pair_index + 3 * group_index
        outputs.append((running[offset + 2] / running[offset + 1][:, None]).astype(jnp.bfloat16))
    attended = jnp.concatenate(outputs, axis=1)
    share = tok_rows // lax.axis_size("tp")
    tp_index = lax.axis_index("tp")
    all_heads = lax.all_gather(attended, "tp", axis=1, tiled=True)
    projected = jnp.dot(all_heads, out_weight, preferred_element_type=jnp.float32)
    stream = (residual.astype(jnp.float32) + projected).astype(jnp.bfloat16)
    normed = normalize(stream, norm_gain)
    stream_own = lax.dynamic_slice_in_dim(stream, tp_index * share, share, 0)
    pieces = (
        lax.all_gather(gate_weight, "sp", axis=0, tiled=True),
        lax.all_gather(value_weight, "sp", axis=0, tiled=True),
    )
    gate_sum = jnp.dot(normed, pieces[0], preferred_element_type=jnp.float32)
    value_sum = jnp.dot(normed, pieces[1], preferred_element_type=jnp.float32)
    gate_pre = gate_sum.astype(jnp.bfloat16)
    value_pre = value_sum.astype(jnp.bfloat16)
    reach = conv_weight.shape[0] // 2
    padded = padded_2(gate_pre, (("sp", 0),), reach)
    mixed_gate = jnp.zeros(gate_pre.shape, jnp.float32)
    for tap in range(conv_weight.shape[0]):
        mixed_gate = mixed_gate + padded[tap : tap + tok_rows].astype(jnp.float32) * conv_weight[
            tap
        ].astype(jnp.float32)
    active = (jax.nn.silu(mixed_gate) * value_pre.astype(jnp.float32)).astype(jnp.bfloat16)
    partial_rows = jnp.dot(
        active,
        lax.all_gather(down_weight, "sp", axis=1, tiled=True),
        preferred_element_type=jnp.float32,
    )
    summed = lax.psum_scatter(
        partial_rows.astype(jnp.bfloat16), "tp", scatter_dimension=0, tiled=True
    ).astype(jnp.float32)
    return (stream_own.astype(jnp.float32) + summed).astype(jnp.bfloat16)


MESH = pl.DeviceIdType.MESH


def layer_kernel(
    zn,
    table_ref,
    q_ref,
    lat_ref,
    key_ref,
    conv_ref,
    expand_hbm,
    res_hbm,
    out_w_hbm,
    gate_hbm,
    value_hbm,
    down_hbm,
    out_ref,
    expand_ref,
    res_ref,
    out_w_ref,
    gate_ref,
    value_ref,
    down_ref,
    lat_all,
    att_send,
    att_recv,
    nrm,
    stage,
    w_full,
    dn_full,
    hbuf,
    abuf,
    halo_send,
    halo_recv,
    part,
    c_send,
    c_recv,
    keep,
    x_send,
    x_recv,
    z_send,
    z_recv,
    in_s,
    lz_s, lz_r, ly_s, ly_r, lc_s, lc_r,
    wz_s, wz_r, wy_s, wy_r,
    dz_s, dz_r, dy_s, dy_r,
    at_s, at_r,
    nz_s, nz_r, nx_s, nx_r, nc_s, nc_r,
    h_s, h_r,
    pc_s, pc_r, px_s, px_r, pz_s, pz_r,
):
    f32, bf16 = jnp.float32, jnp.bfloat16
    s, t = lax.axis_index("sp"), lax.axis_index("tp")
    z, y = s // 2, s % 2
    x, c = t // 2, t % 2
    yo, xo, co = 1 - y, 1 - x, 1 - c
    rows = lat_ref.shape[0]
    half, share = rows // 2, rows // 4
    rank = lat_ref.shape[1]
    sub = down_ref.shape[0] // zn
    sp = 2 * zn

    def to_z(d):
        return {"sp": 2 * ((z + d) % zn) + y, "tp": t}

    y_dev = {"sp": 2 * z + yo, "tp": t}
    x_dev = {"sp": s, "tp": 2 * xo + c}
    c_dev = {"sp": s, "tp": 2 * x + co}

    def from_z(d):
        return (z + zn - d) % zn

    started = []

    def send(src, dst, s_sem, r_sem, dev):
        copy = pltpu.make_async_remote_copy(
            src_ref=src, dst_ref=dst, send_sem=s_sem, recv_sem=r_sem,
            device_id=dev, device_id_type=MESH,
        )
        copy.start()
        started.append(copy)
        return copy

    def arrived(dst, s_sem, r_sem):
        pltpu.make_async_remote_copy(
            src_ref=dst, dst_ref=dst, send_sem=s_sem, recv_sem=r_sem,
            device_id=c_dev, device_id_type=MESH,
        ).wait_recv()

    barrier = pltpu.get_barrier_semaphore()
    partners = [to_z(d) for d in range(1, zn)] + [y_dev, x_dev, c_dev, {"sp": s, "tp": 2 * xo + co}]
    for dev in partners:
        pl.semaphore_signal(barrier, inc=1, device_id=dev, device_id_type=MESH)

    mine_rows = pl.ds(pl.multiple_of(t * share, share), share)
    loads = [
        pltpu.make_async_copy(src, dst, in_s.at[i])
        for i, (src, dst) in enumerate(
            [
                (gate_hbm, gate_ref),
                (value_hbm, value_ref),
                (down_hbm, down_ref),
                (expand_hbm, expand_ref),
                (res_hbm.at[mine_rows, :], res_ref),
                (out_w_hbm, out_w_ref),
            ]
        )
    ]
    for load in loads:
        load.start()

    h = ROPE // 2
    cos, sine = table_ref[:h, :], table_ref[h:ROPE, :]

    def turn(v):
        a, b = v[:h], v[h:]
        return jnp.concatenate([a * cos - b * sine, b * cos + a * sine], axis=0)

    rot = NOPE_A + NOPE_B
    q = q_ref[...].astype(f32)
    pair = jnp.concatenate([turn(q[rot + ROPE :]), turn(key_ref[...].astype(f32))], axis=0).T.astype(bf16)
    q_narrow_t, key_turned = pair[:, :ROPE], pair[:, ROPE:]
    for i in range(2):
        lat_all[s, i, :, :rank] = lat_ref[i * half : (i + 1) * half, :]
        lat_all[s, i, :, rank : rank + ROPE] = key_turned[i * half : (i + 1) * half, :]
        lat_all[s, i, :, rank + ROPE :] = jnp.zeros((half, ROPE), bf16)
    pl.semaphore_wait(barrier, len(partners))

    mine = lat_all.at[s, c]
    for d in range(1, zn):
        send(mine, mine, lz_s.at[d], lz_r.at[d], to_z(d))
    send(mine, mine, ly_s.at[0], ly_r.at[0], y_dev)

    loads[0].wait()
    loads[1].wait()
    for k in range(zn):
        stage[k, :, :sub] = gate_ref[:, k * sub : (k + 1) * sub]
        stage[k, :, sub:] = value_ref[:, k * sub : (k + 1) * sub]
    for d in range(1, zn):
        send(stage.at[(z + d) % zn], w_full.at[s], wz_s.at[d], wz_r.at[d], to_z(d))
    w_full[s] = stage[z]
    loads[2].wait()

    def send_down(d):
        zz = (z + d) % zn
        piece = down_ref.at[pl.ds(pl.multiple_of(zz * sub, sub), sub), :]
        send(piece, dn_full.at[s], dz_s.at[d], dz_r.at[d], to_z(d))

    send_down(1)
    dn_full[s] = down_ref[pl.ds(pl.multiple_of(z * sub, sub), sub), :]

    for d in range(1, zn):
        blk = lat_all.at[2 * from_z(d) + y, c]
        arrived(blk, lz_s.at[d], lz_r.at[d])
        send(blk, blk, ly_s.at[d], ly_r.at[d], y_dev)
        send(blk, blk, lc_s.at[d], lc_r.at[d], c_dev)
    send(w_full.at[s], w_full.at[s], wy_s.at[0], wy_r.at[0], y_dev)
    for d in range(zn):
        blk = lat_all.at[2 * from_z(d) + yo, c]
        arrived(blk, ly_s.at[d], ly_r.at[d])
        send(blk, blk, lc_s.at[zn + d], lc_r.at[zn + d], c_dev)
    q_wide = q[:NOPE_A].T.astype(bf16)
    pair = jnp.concatenate([q[NOPE_A:rot], turn(q[rot : rot + ROPE])], axis=0).T.astype(bf16)
    q_narrow, q_wide_t = pair[:, :NOPE_B], pair[:, NOPE_B:]
    loads[3].wait()
    for d in range(1, zn):
        arrived(lat_all.at[2 * from_z(d) + y, co], lc_s.at[d], lc_r.at[d])
    for d in range(zn):
        arrived(lat_all.at[2 * from_z(d) + yo, co], lc_s.at[zn + d], lc_r.at[zn + d])

    whole = lat_all[...].reshape(sp * rows, lat_all.shape[3])
    expanded = jnp.dot(whole[:, :rank], expand_ref[...], preferred_element_type=f32).astype(bf16)
    keys_t = whole[:, rank : rank + ROPE]

    def attend(qc, qt, kc, v, scale):
        dims = (((1,), (1,)), ((), ()))
        scores = (
            lax.dot_general(qc, kc, dims, preferred_element_type=f32)
            + lax.dot_general(qt, keys_t, dims, preferred_element_type=f32)
        ) * scale
        w = jnp.exp(scores - jnp.max(scores, axis=1, keepdims=True))
        total = jnp.sum(w, axis=1, keepdims=True)
        return (jnp.dot(w.astype(bf16), v, preferred_element_type=f32) / total).astype(bf16)

    nb = NOPE_A + VAL_A
    wide = attend(q_wide, q_wide_t, expanded[:, :NOPE_A], expanded[:, NOPE_A:nb], (NOPE_A + ROPE) ** -0.5)
    narrow = attend(
        q_narrow, q_narrow_t, expanded[:, nb : nb + NOPE_B],
        expanded[:, nb + NOPE_B : nb + NOPE_B + VAL_B], (NOPE_B + ROPE) ** -0.5,
    )
    vals = VAL_A + VAL_B
    for i in range(4):
        att_send[i, :, :VAL_A] = wide[i * share : (i + 1) * share, :]
        att_send[i, :, VAL_A:vals] = narrow[i * share : (i + 1) * share, :]
    others = [(2 * x + co), (2 * xo + c), (2 * xo + co)]
    for i, o in enumerate(others):
        send(att_send.at[o], att_recv.at[t], at_s.at[i], at_r.at[i], {"sp": s, "tp": o})
    att_recv[t] = att_send[t]

    def forward(full, sz, rz, sy, ry, d):
        blk = full.at[2 * from_z(d) + y]
        arrived(blk, sz.at[d], rz.at[d])
        send(blk, blk, sy.at[d], ry.at[d], y_dev)

    def forward_weights(d):
        forward(w_full, wz_s, wz_r, wy_s, wy_r, d)

    loads[4].wait()
    loads[5].wait()
    for i, o in enumerate(others):
        arrived(att_recv.at[o], at_s.at[i], at_r.at[i])
    projected = jnp.dot(att_recv[0, :, :vals], out_w_ref[:vals, :], preferred_element_type=f32)
    for i in range(1, 4):
        projected += jnp.dot(
            att_recv[i, :, :vals], out_w_ref[i * vals : (i + 1) * vals, :], preferred_element_type=f32
        )
    stream = (res_ref[...].astype(f32) + projected).astype(bf16)
    stream_f = stream.astype(f32)
    scaled = stream_f * lax.rsqrt(jnp.mean(stream_f * stream_f, axis=1, keepdims=True) + 1e-06)
    for k in range(scaled.shape[1] // rows):
        gain = table_ref[ROPE + k : ROPE + k + 1, :]
        nrm[z, t, :, k * rows : (k + 1) * rows] = (scaled[:, k * rows : (k + 1) * rows] * gain).astype(bf16)

    own = nrm.at[z, t]
    for d in range(1, zn):
        send(own, own, nz_s.at[d], nz_r.at[d], to_z(d))
    send(own, own, nx_s.at[0], nx_r.at[0], x_dev)
    send(own, own, nc_s.at[0], nc_r.at[0], c_dev)
    for d in range(2, zn):
        send_down(d)
    forward_weights(1)
    xt = 2 * xo + c
    blk = nrm.at[z, xt]
    arrived(blk, nx_s.at[0], nx_r.at[0])
    send(blk, blk, nc_s.at[zn], nc_r.at[zn], c_dev)
    for d in range(1, zn):
        blk = nrm.at[from_z(d), t]
        arrived(blk, nz_s.at[d], nz_r.at[d])
        send(blk, blk, nx_s.at[d], nx_r.at[d], x_dev)
        send(blk, blk, nc_s.at[d], nc_r.at[d], c_dev)
        if d > 1:
            forward_weights(d)
    for d in range(1, zn):
        blk = nrm.at[from_z(d), xt]
        arrived(blk, nx_s.at[d], nx_r.at[d])
        send(blk, blk, nc_s.at[zn + d], nc_r.at[zn + d], c_dev)
    send(dn_full.at[s], dn_full.at[s], dy_s.at[0], dy_r.at[0], y_dev)
    forward(dn_full, dz_s, dz_r, dy_s, dy_r, 1)
    for d in range(zn):
        arrived(w_full.at[2 * from_z(d) + yo], wy_s.at[d], wy_r.at[d])
    weights = w_full[...].reshape(sp * w_full.shape[1], 2 * sub)
    for d in range(zn):
        zz = from_z(d)
        arrived(nrm.at[zz, 2 * x + co], nc_s.at[d], nc_r.at[d])
        arrived(nrm.at[zz, 2 * xo + co], nc_s.at[zn + d], nc_r.at[zn + d])
        block = nrm[zz].reshape(rows, nrm.shape[3])
        hbuf[zz] = jnp.dot(block, weights, preferred_element_type=f32).astype(bf16)

    wide_lanes = halo_send.shape[1]
    for k in range(zn):
        g = hbuf[k, :, :wide_lanes].astype(f32)
        halo_send[k : k + 1, :] = g[rows - 1 : rows, :]
        halo_send[zn + k : zn + k + 1, :] = g[0:1, :]
    send(halo_send, halo_recv, h_s.at[0], h_r.at[0], y_dev)
    for d in range(2, zn):
        forward(dn_full, dz_s, dz_r, dy_s, dy_r, d)
    taps = jnp.zeros((conv_ref.shape[0], wide_lanes), f32)
    conv_all = conv_ref[...].astype(f32)
    pieces = [conv_all[:, k * sub : (k + 1) * sub] for k in range(zn)]
    taps = pieces[0]
    for k in range(1, zn):
        taps = jnp.where(z == k, pieces[k], taps)
    taps = jnp.concatenate([taps, jnp.zeros((taps.shape[0], wide_lanes - sub), f32)], axis=1)
    row_id = lax.broadcasted_iota(jnp.int32, (rows, wide_lanes), 0)
    arrived(halo_recv, h_s.at[0], h_r.at[0])
    nothing = jnp.zeros((1, wide_lanes), f32)
    for k in range(zn):
        before_low = halo_recv[k - 1 : k, :] if k > 0 else nothing
        before = jnp.where(y == 0, before_low, halo_recv[k : k + 1, :])
        after_high = halo_recv[zn + k + 1 : zn + k + 2, :] if k < zn - 1 else nothing
        after = jnp.where(y == 0, halo_recv[zn + k : zn + k + 1, :], after_high)
        g = hbuf[k, :, :wide_lanes].astype(f32)
        up = jnp.where(row_id == 0, before, pltpu.roll(g, 1, 0))
        down = jnp.where(row_id == rows - 1, after, pltpu.roll(g, rows - 1, 0))
        mixed = up * taps[0:1] + g * taps[1:2] + down * taps[2:3]
        mixed = mixed[:, :sub]
        v = hbuf[k].astype(f32)[:, sub:]
        abuf[k] = (mixed / (1.0 + jnp.exp(-mixed)) * v).astype(bf16)

    for d in range(zn):
        arrived(dn_full.at[2 * from_z(d) + yo], dy_s.at[d], dy_r.at[d])
    order = list(range(1, zn)) + [0]
    depth = dn_full.shape[2]
    for d in order:
        zz = (z + d) % zn
        a = abuf[zz]
        for k in range(sp):
            p = jnp.dot(a, dn_full[k], preferred_element_type=f32)
            part[d, :, :, k * depth : (k + 1) * depth] = p.reshape(4, share, depth)
        for i in range(2):
            c_send[d, i] = part[d, 2 * i + co].astype(bf16)
        send(c_send.at[d], c_recv.at[d], pc_s.at[d], pc_r.at[d], c_dev)
    for d in order:
        arrived(c_recv.at[d], pc_s.at[d], pc_r.at[d])
        x_send[d] = (part[d, 2 * xo + c] + c_recv[d, xo].astype(f32)).astype(bf16)
        send(x_send.at[d], x_recv.at[d], px_s.at[d], px_r.at[d], x_dev)
        keep[d] = part[d, 2 * x + c] + c_recv[d, x].astype(f32)
    for d in order:
        arrived(x_recv.at[d], px_s.at[d], px_r.at[d])
        if d > 0:
            z_send[d] = (keep[d] + x_recv[d].astype(f32)).astype(bf16)
            send(z_send.at[d], z_recv.at[d], pz_s.at[d], pz_r.at[d], to_z(d))
    total = keep[0] + x_recv[0].astype(f32)
    for d in range(1, zn):
        arrived(z_recv.at[d], pz_s.at[d], pz_r.at[d])
        total += z_recv[d].astype(f32)
    out_ref[...] = (stream_f + total).astype(bf16)
    for copy in started:
        copy.wait_send()


def kernel_body(zn, *args):
    (queries, latents, shared_key, expand_weight, residual, out_weight, norm_gain,
     gate_weight, value_weight, conv_weight, down_weight) = args
    rows, width = residual.shape
    sub = down_weight.shape[0] // zn
    share, half = rows // 4, rows // 2
    d_own = gate_weight.shape[0]
    positions = lax.axis_index("sp") * rows + jnp.arange(rows, dtype=jnp.int32)
    cos_table, sine_table = tables(positions, ROPE)
    gain = norm_gain.reshape(width // rows, rows).astype(jnp.float32)
    table = jnp.concatenate([cos_table.T, sine_table.T, gain], axis=0)
    bf16, f32 = jnp.bfloat16, jnp.float32
    vals = VAL_A + VAL_B
    lanes = -(-vals // 128) * 128
    halo_lanes = -(-sub // 128) * 128
    V, DMA = pltpu.VMEM, pltpu.SemaphoreType.DMA
    sems = [DMA((6,))]
    for count in (zn, zn, 2 * zn, zn, zn, zn, zn, 3, zn, zn, 2 * zn, 1, zn, zn, zn):
        sems += [DMA((count,)), DMA((count,))]
    return pl.pallas_call(
        functools.partial(layer_kernel, zn),
        out_shape=jax.ShapeDtypeStruct((share, width), bf16),
        in_specs=[pl.BlockSpec(memory_space=V)] * 5 + [pl.BlockSpec(memory_space=pl.ANY)] * 6,
        out_specs=pl.BlockSpec(memory_space=V),
        scratch_shapes=[
            V(expand_weight.shape, bf16),
            V((share, width), bf16),
            V(out_weight.shape, bf16),
            V(gate_weight.shape, bf16),
            V(value_weight.shape, bf16),
            V(down_weight.shape, bf16),
            V((2 * zn, 2, half, latents.shape[1] + 2 * ROPE), bf16),
            V((4, share, lanes), bf16),
            V((4, share, lanes), bf16),
            V((zn, 4, share, width), bf16),
            V((zn, d_own, 2 * sub), bf16),
            V((2 * zn, d_own, 2 * sub), bf16),
            V((2 * zn, sub, down_weight.shape[1]), bf16),
            V((zn, rows, 2 * sub), bf16),
            V((zn, rows, sub), bf16),
            V((2 * zn, halo_lanes), f32),
            V((2 * zn, halo_lanes), f32),
            V((zn, 4, share, width), f32),
            V((zn, 2, share, width), bf16),
            V((zn, 2, share, width), bf16),
            V((zn, share, width), f32),
            V((zn, share, width), bf16),
            V((zn, share, width), bf16),
            V((zn, share, width), bf16),
            V((zn, share, width), bf16),
        ] + sems,
        compiler_params=pltpu.CompilerParams(collective_id=0, has_side_effects=True),
    )(table, queries.T, latents, shared_key.T, conv_weight, expand_weight, residual, out_weight,
      gate_weight, value_weight, down_weight)


def pick(*args):
    zn = lax.axis_size("sp") // 2
    hidden = args[10].shape[0]
    sub = hidden // zn
    fits = (
        lax.axis_size("sp") % 2 == 0
        and lax.axis_size("tp") == 4
        and hidden % zn == 0
        and sub % 64 == 0
        and args[7].shape[0] % 128 == 0
        and args[0].shape[0] % 128 == 0
        and args[4].shape[1] % args[0].shape[0] == 0
        and args[9].shape[0] == 3
    )
    return kernel_body(zn, *args) if fits else body(*args)


def solution(mesh):
    in_specs = (
        P("sp", "tp"),
        P("sp", None),
        P("sp", None),
        P(None, "tp"),
        P("sp", None),
        P(),
        P(),
        P("sp", "tp"),
        P("sp", "tp"),
        P(None, "tp"),
        P("tp", "sp"),
    )
    out_specs = P(("sp", "tp"), None)
    return jax.shard_map(pick, mesh=mesh, in_specs=in_specs, out_specs=out_specs, check_vma=False)
```
